32 devices in a mesh: fs: 8 (over z, y), tp: 4 (over x, core).
Axes of the slice: x: 2, y: 2, z: 4, core: 2. Of those that a mesh axis runs over, the one named last changes fastest.
Arguments:
- layer_input: bfloat16 [20480, 4096], P('fs'), may hold values from -140 to 140
- query_cotangent: bfloat16 [20480, 2048], P('fs', 'tp'), may hold values from -0.46817673 to 0.46817673
- value_cotangent: bfloat16 [20480, 512], P('fs', 'tp'), may hold values from -0.46817673 to 0.46817673
- query_weight: float32 [4096, 2048], P('fs', 'tp'), may hold values from -0.09375 to 0.09375
- value_weight: float32 [4096, 512], P('fs', 'tp'), may hold values from -0.09375 to 0.09375
- query_moment: float32 [4096, 2048], P('fs', 'tp'), may hold values from -18 to 18
- value_moment: float32 [4096, 512], P('fs', 'tp'), may hold values from -18 to 18
- query_left_stat: float32 [16, 256, 256], P('fs'), may hold values from -24 to 24
- value_left_stat: float32 [16, 256, 256], P('fs'), may hold values from -24 to 24
- query_right_stat: float32 [32, 64, 64], P('tp'), may hold values from -24 to 24
- value_right_stat: float32 [8, 64, 64], P('tp'), may hold values from -24 to 24
- query_left_root: bfloat16 [16, 256, 256], P('fs'), may hold values from -1.5 to 2
- value_left_root: bfloat16 [16, 256, 256], P('fs'), may hold values from -1.5 to 2
- query_right_root: bfloat16 [32, 64, 64], P('tp'), may hold values from -1.5 to 2
- value_right_root: bfloat16 [8, 64, 64], P('tp'), may hold values from -1.5 to 2
Outputs:
- query_update: float32 [4096, 2048], P('fs', 'tp')
- value_update: float32 [4096, 512], P('fs', 'tp')
- query_moment_new: float32 [4096, 2048], P('fs', 'tp')
- value_moment_new: float32 [4096, 512], P('fs', 'tp')
- query_left_new: float32 [16, 256, 256], P('fs')
- value_left_new: float32 [16, 256, 256], P('fs')
- query_right_new: float32 [32, 64, 64], P('tp')
- value_right_new: float32 [8, 64, 64], P('tp')
- query_copy: bfloat16 [4096, 2048], P(None, 'tp')
- value_copy: bfloat16 [4096, 512], P(None, 'tp')
The draws below stay inside these ranges and needn't reach their ends.
All inputs are finite; a program needn't handle non-finite values.
Results may differ from the reference program's by a relative error of at most 0.0075.
Values may be sent and summed in bfloat16 or wider, within the bound.
A program may use at most 128 MiB of HBM per device.

```python
import jax
import jax.numpy as jnp
from jax import lax

D = 4096
HEADS = 32
KV_HEADS = 8
HEAD = 64
BLOCK = 256
TOKENS = 20480
Q_COLS = 2048
V_COLS = 512


def scaled_draw(key, row_count, columns, base_scale):
    noise_key, scale_key = jax.random.split(key, 2)
    column_ramp = jnp.arange(columns, dtype=jnp.float32) / columns
    jitter = jax.random.uniform(scale_key, (columns,), jnp.float32)
    noise = jnp.clip(jax.random.normal(noise_key, (row_count, columns), jnp.float32), -6.0, 6.0)
    exponent = 0.5 * column_ramp + 0.5 * jitter
    return (noise * (base_scale * 10.0 ** exponent)).astype(jnp.bfloat16)


def root_draw(key, matrix_count, order):
    diag_key, off_key = jax.random.split(key, 2)
    diagonal = jax.random.uniform(diag_key, (matrix_count, order), jnp.float32, 0.6, 1.4)
    spread = jnp.clip(jax.random.normal(off_key, (matrix_count, order, order), jnp.float32), -4.0, 4.0)
    spread = spread * (0.6 / order ** 0.5)
    spread = 0.5 * (spread + jnp.swapaxes(spread, 1, 2))
    identity = jnp.eye(order, dtype=jnp.float32)
    return (spread * (1.0 - identity) + diagonal[:, :, None] * identity).astype(jnp.bfloat16)


def draw_layer_input(key, part):
    return scaled_draw(jax.random.fold_in(key, 11), TOKENS, D, 1.0)


def draw_query_cotangent(key, part):
    return scaled_draw(jax.random.fold_in(key, 12), TOKENS, Q_COLS, 0.5 / TOKENS ** 0.5)


def draw_value_cotangent(key, part):
    return scaled_draw(jax.random.fold_in(key, 13), TOKENS, V_COLS, 0.5 / TOKENS ** 0.5)


def draw_query_left_root(key, part):
    return root_draw(jax.random.fold_in(key, 21), D // BLOCK, BLOCK)


def draw_value_left_root(key, part):
    return root_draw(jax.random.fold_in(key, 22), D // BLOCK, BLOCK)


def draw_query_right_root(key, part):
    return root_draw(jax.random.fold_in(key, 23), HEADS, HEAD)


def draw_value_right_root(key, part):
    return root_draw(jax.random.fold_in(key, 24), KV_HEADS, HEAD)


def levels(rng, extent, shards, least, top_value):
    def one(dim, shards_of):
        steps = jax.random.uniform(jax.random.fold_in(jax.random.fold_in(rng, 6), dim), (shards_of,), jnp.float32, least / len(shards), top_value / len(shards))
        return jnp.repeat(jnp.exp(steps), extent[dim] // shards_of).reshape((-1,) + (1,) * (len(extent) - dim - 1))

    level = one(*shards[0])
    for cut in shards[1:]:
        level = level * one(*cut)
    return level


def normal_values(own_key, dims, width, reach, shards=(), held_as=jnp.bfloat16):
    result = width * jax.random.normal(own_key, dims, jnp.float32)
    if shards:
        result = result * levels(own_key, dims, shards, -0.22, 0.18)
    return jnp.clip(result, -reach, reach).astype(held_as)


def setup_inputs(seed: int = 0) -> dict:
    keys = jax.random.split(jax.random.key(seed), 16)
    layer_input = draw_layer_input(jax.random.fold_in(keys[15], 71), 0)
    query_cotangent = draw_query_cotangent(jax.random.fold_in(keys[15], 71), 0)
    value_cotangent = draw_value_cotangent(jax.random.fold_in(keys[15], 71), 0)
    query_weight = normal_values(keys[3], (D, Q_COLS), D ** -0.5, 0.09375, ((0, 8), (1, 4)), jnp.float32)
    value_weight = normal_values(keys[4], (D, V_COLS), D ** -0.5, 0.09375, ((0, 8), (1, 4)), jnp.float32)
    query_moment = normal_values(keys[5], (D, Q_COLS), 3.0, 18.0, ((0, 8), (1, 4)), jnp.float32)
    value_moment = normal_values(keys[6], (D, V_COLS), 3.0, 18.0, ((0, 8), (1, 4)), jnp.float32)
    query_left_stat = normal_values(keys[7], (D // BLOCK, BLOCK, BLOCK), 4.0, 24.0, ((0, 8),), jnp.float32)
    value_left_stat = normal_values(keys[8], (D // BLOCK, BLOCK, BLOCK), 4.0, 24.0, ((0, 8),), jnp.float32)
    query_right_stat = normal_values(keys[9], (HEADS, HEAD, HEAD), 4.0, 24.0, ((0, 4),), jnp.float32)
    value_right_stat = normal_values(keys[10], (KV_HEADS, HEAD, HEAD), 4.0, 24.0, ((0, 4),), jnp.float32)
    query_left_root = draw_query_left_root(jax.random.fold_in(keys[15], 71), 0)
    value_left_root = draw_value_left_root(jax.random.fold_in(keys[15], 71), 0)
    query_right_root = draw_query_right_root(jax.random.fold_in(keys[15], 71), 0)
    value_right_root = draw_value_right_root(jax.random.fold_in(keys[15], 71), 0)
    return {"layer_input": layer_input, "query_cotangent": query_cotangent, "value_cotangent": value_cotangent, "query_weight": query_weight, "value_weight": value_weight, "query_moment": query_moment, "value_moment": value_moment, "query_left_stat": query_left_stat, "value_left_stat": value_left_stat, "query_right_stat": query_right_stat, "value_right_stat": value_right_stat, "query_left_root": query_left_root, "value_left_root": value_left_root, "query_right_root": query_right_root, "value_right_root": value_right_root}


momentum_decay = 0.9
statistic_decay = 0.9
learning_rate = 0.002
epsilon = 1e-06
highest = lax.Precision.HIGHEST

def token_sum(inputs, cotangent):
    return lax.dot_general(inputs, cotangent, (((0,), (0,)), ((), ())), preferred_element_type=jnp.float32)

def precondition(moment, left_root, right_root):
    total_rows, columns = moment.shape
    head_count = columns // HEAD
    by_head = jnp.einsum('rhk,hkl->rhl', moment.reshape(total_rows, head_count, HEAD), right_root.astype(jnp.float32), precision=highest)
    by_block = by_head.reshape(total_rows // BLOCK, BLOCK, columns)
    return jnp.einsum('bij,bjc->bic', left_root.astype(jnp.float32), by_block, precision=highest).reshape(total_rows, columns)

def update_matrix(gradient, weight, moment, left_stat, right_stat, left_root, right_root):
    total_rows, columns = gradient.shape
    moment_new = momentum_decay * moment + (1.0 - momentum_decay) * gradient
    blocks = gradient.reshape(total_rows // BLOCK, BLOCK, columns)
    left_sum = jnp.einsum('bic,bjc->bij', blocks, blocks, precision=highest)
    left_new = statistic_decay * left_stat + (1.0 - statistic_decay) / columns * left_sum
    per_head = gradient.reshape(total_rows, columns // HEAD, HEAD)
    right_sum = jnp.einsum('rhk,rhl->hkl', per_head, per_head, precision=highest)
    right_new = statistic_decay * right_stat + (1.0 - statistic_decay) / total_rows * right_sum
    direction = precondition(moment_new, left_root, right_root)
    graft_scale = jnp.sqrt(jnp.sum(moment_new * moment_new) / (jnp.sum(direction * direction) + epsilon))
    update = graft_scale * direction
    weight_copy = (weight - learning_rate * update).astype(jnp.bfloat16)
    return (update, moment_new, left_new, right_new, weight_copy)

def reference(layer_input, query_cotangent, value_cotangent, query_weight, value_weight, query_moment, value_moment, query_left_stat, value_left_stat, query_right_stat, value_right_stat, query_left_root, value_left_root, query_right_root, value_right_root):
    query_gradient = token_sum(layer_input, query_cotangent)
    value_gradient = token_sum(layer_input, value_cotangent)
    query_parts = update_matrix(query_gradient, query_weight, query_moment, query_left_stat, query_right_stat, query_left_root, query_right_root)
    value_parts = update_matrix(value_gradient, value_weight, value_moment, value_left_stat, value_right_stat, value_left_root, value_right_root)
    return (query_parts[0], value_parts[0], query_parts[1], value_parts[1], query_parts[2], value_parts[2], query_parts[3], value_parts[3], query_parts[4], value_parts[4])
```

```python
import functools

import jax
import jax.numpy as jnp
from jax import lax
from jax.experimental import pallas as pl
from jax.experimental.pallas import tpu as pltpu
from jax.sharding import PartitionSpec as P

MESH = pl.DeviceIdType.MESH
f32 = jnp.float32
bf16 = jnp.bfloat16

momentum_decay = 0.9
statistic_decay = 0.9
learning_rate = 0.002
epsilon = 1e-06


def grid_of(fs):
    nz = 4 if fs % 4 == 0 else 1
    return nz, fs // nz


def greet(peers):
    barrier = pltpu.get_barrier_semaphore()
    for peer in peers:
        pl.semaphore_signal(barrier, inc=1, device_id=peer, device_id_type=MESH)
    pl.semaphore_wait(barrier, len(peers))


def remote(src, dst, send_sem, recv_sem, peer):
    return pltpu.make_async_remote_copy(
        src_ref=src,
        dst_ref=dst,
        send_sem=send_sem,
        recv_sem=recv_sem,
        device_id=peer,
        device_id_type=MESH,
    )


def mix(moment, gradient):
    return momentum_decay * moment + (1.0 - momentum_decay) * gradient


def gradient_kernel(
    nz,
    ny,
    cot_ref,
    x_ref,
    out_ref,
    xbuf,
    far,
    far_in,
    near,
    hop,
    hop_in,
    x_sem,
    y_send,
    y_recv,
    z_send,
    z_recv,
):
    me, tp = lax.axis_index("fs"), lax.axis_index("tp")
    z, y = me // ny, me % ny
    rows = out_ref.shape[1]
    chunks, far_count = nz * ny, nz * (ny - 1)
    slots = xbuf.shape[0]

    def owner(i):
        return ((z + i % nz + 1) % nz) * ny + (y + i // nz + 1) % ny

    def fetch(i):
        columns = pl.ds(pl.multiple_of(owner(i) * rows, 128), rows)
        return pltpu.make_async_copy(
            x_ref.at[:, columns], xbuf.at[i % slots], x_sem.at[i % slots]
        )

    def y_copy(i):
        peer = (z * ny + (y + i // nz + 1) % ny, tp)
        return remote(far.at[i], far_in.at[i], y_send.at[i], y_recv.at[i], peer)

    def z_copy(k):
        peer = (((z + k + 1) % nz) * ny + y, tp)
        return remote(hop.at[k], hop_in.at[k], z_send.at[k], z_recv.at[k], peer)

    for i in range(slots - 1):
        fetch(i).start()
    peers = [(z * ny + (y + d) % ny, tp) for d in range(1, ny)]
    peers += [(((z + d) % nz) * ny + y, tp) for d in range(1, nz)]
    greet(peers)

    width = min(rows, 256)

    def multiply(i, keep):
        @pl.when(i + slots - 1 < chunks)
        def _():
            fetch(i + slots - 1).start()

        fetch(i).wait()
        for j in range(rows // width):
            part = jnp.dot(
                cot_ref[...],
                xbuf[i % slots, :, j * width : (j + 1) * width],
                preferred_element_type=f32,
            )
            keep(i, slice(j * width, (j + 1) * width), part)

    def far_step(i, carry):
        def keep(i, columns, part):
            far[i, :, columns] = part.astype(bf16)

        multiply(i, keep)
        y_copy(i).start()
        return carry

    def near_step(i, carry):
        def keep(i, columns, part):
            near[i - far_count, :, columns] = part

        multiply(i, keep)
        return carry

    lax.fori_loop(0, far_count, far_step, 0)
    lax.fori_loop(far_count, chunks, near_step, 0)

    for k in range(nz):
        for d in range(ny - 1):
            y_copy(d * nz + k).wait_recv()
        total = near[k]
        for d in range(ny - 1):
            total = total + far_in[d * nz + k].astype(f32)
        if k < nz - 1:
            hop[k] = total.astype(bf16)
            z_copy(k).start()
        else:
            out_ref[...] = total
    for k in range(nz - 1):
        z_copy(k).wait_recv()
        out_ref[...] += hop_in[k].astype(f32)
    for i in range(far_count):
        y_copy(i).wait_send()
    for k in range(nz - 1):
        z_copy(k).wait_send()


def gradients_of_rows(nz, ny, cotangent, layer_input):
    columns, tokens = cotangent.shape
    rows = layer_input.shape[1] // (nz * ny)
    far_count = nz * (ny - 1)
    return pl.pallas_call(
        functools.partial(gradient_kernel, nz, ny),
        out_shape=jax.ShapeDtypeStruct((columns, rows), f32),
        in_specs=[
            pl.BlockSpec(memory_space=pltpu.VMEM),
            pl.BlockSpec(memory_space=pl.ANY),
        ],
        out_specs=pl.BlockSpec(memory_space=pltpu.VMEM),
        scratch_shapes=[
            pltpu.VMEM((3, tokens, rows), bf16),
            pltpu.VMEM((far_count, columns, rows), bf16),
            pltpu.VMEM((far_count, columns, rows), bf16),
            pltpu.VMEM((nz, columns, rows), f32),
            pltpu.VMEM((nz - 1, columns, rows), bf16),
            pltpu.VMEM((nz - 1, columns, rows), bf16),
            pltpu.SemaphoreType.DMA((3,)),
            pltpu.SemaphoreType.DMA((far_count,)),
            pltpu.SemaphoreType.DMA((far_count,)),
            pltpu.SemaphoreType.DMA((nz - 1,)),
            pltpu.SemaphoreType.DMA((nz - 1,)),
        ],
        compiler_params=pltpu.CompilerParams(collective_id=0, has_side_effects=True),
    )(cotangent, layer_input)


def dot_split(left, right, split_left):
    wide = left if split_left else right
    high = wide.astype(bf16)
    low = (wide - high.astype(f32)).astype(bf16)
    if split_left:
        return jnp.dot(high, right, preferred_element_type=f32) + jnp.dot(
            low, right, preferred_element_type=f32
        )
    return jnp.dot(left, high, preferred_element_type=f32) + jnp.dot(
        left, low, preferred_element_type=f32
    )


def outer(a):
    return lax.dot_general(a, a, (((1,), (1,)), ((), ())), preferred_element_type=f32)


def total_of(x):
    return jnp.sum(jnp.sum(x, axis=0, keepdims=True), axis=1, keepdims=True)


def update_kernel(
    nz,
    ny,
    ntp,
    grad_ref,
    weight_q,
    weight_v,
    moment_q,
    moment_v,
    left_stat_q,
    left_stat_v,
    right_stat_q,
    right_stat_v,
    left_root_q,
    left_root_v,
    right_root_q,
    right_root_v,
    update_q,
    update_v,
    moment_new_q,
    moment_new_v,
    left_new_q,
    left_new_v,
    right_new_q,
    right_new_v,
    copy_q,
    copy_v,
    left_terms,
    right_terms,
    tp_squares,
    fs_squares,
    tp_sems,
    fs_sems,
    left_sems,
    right_sems,
    z_sems,
    y_sems,
):
    nfs = nz * ny
    me, tp = lax.axis_index("fs"), lax.axis_index("tp")
    z, y = me // ny, me % ny
    rows, width_q = moment_q.shape
    width_v = moment_v.shape[1]
    blocks, block = left_root_q.shape[:2]
    head = right_stat_q.shape[1]
    heads_q, heads_v = right_stat_q.shape[0], right_stat_v.shape[0]

    tp_peers = [(me, (tp + d) % ntp) for d in range(1, ntp)]
    fs_peers = [((me + d) % nfs, tp) for d in range(1, nfs)]

    def direction(grad, moment, moment_new, left_root, right_root, update):
        new = mix(moment[...], grad)
        moment_new[...] = new
        turned = dot_split(new, right_root[...], True)
        squares = jnp.zeros((1, 1), f32)
        for b in range(blocks):
            part = dot_split(left_root[b], turned[b * block : (b + 1) * block], False)
            update[b * block : (b + 1) * block, :] = part
            squares = squares + total_of(part * part)
        return total_of(new * new), squares

    grad_q = grad_ref[:width_q, :].T
    grad_v = grad_ref[width_q:, :].T
    sums = direction(grad_q, moment_q, moment_new_q, left_root_q, right_root_q, update_q)
    sums += direction(grad_v, moment_v, moment_new_v, left_root_v, right_root_v, update_v)
    row = lax.broadcasted_iota(jnp.int32, (8, 128), 0)
    tile = jnp.zeros((8, 128), f32)
    for i, one in enumerate(sums):
        tile = jnp.where(row == i, one, tile)
    tp_squares[tp] = tile

    greet(tp_peers + fs_peers)

    def spread(buffer, own, sems, peers):
        return [
            remote(buffer.at[own], buffer.at[own], sems.at[0, d], sems.at[1, d], peer)
            for d, peer in enumerate(peers)
        ]

    tp_copies = spread(tp_squares, tp, tp_sems, tp_peers)
    fs_copies = spread(fs_squares, me, fs_sems, fs_peers)
    left_copies = spread(left_terms, tp, left_sems, tp_peers)
    right_copies = spread(right_terms, me, right_sems, fs_peers)

    for copy in tp_copies:
        copy.start()
    for grad, first in ((grad_q, 0), (grad_v, blocks)):
        narrow = grad.astype(bf16)
        for b in range(blocks):
            left_terms[tp, first + b] = outer(narrow[b * block : (b + 1) * block]).astype(bf16)
    for h in range(heads_q + heads_v):
        right_terms[me, h] = outer(grad_ref[h * head : (h + 1) * head, :].astype(bf16)).astype(bf16)
    for copy in tp_copies:
        copy.wait_recv()
    tile = tp_squares[0]
    for i in range(1, ntp):
        tile = tile + tp_squares[i]
    fs_squares[me] = tile
    for copy in fs_copies + left_copies + right_copies:
        copy.start()
    for copy in fs_copies:
        copy.wait_recv()
    tile = fs_squares[0]
    for i in range(1, nfs):
        tile = tile + fs_squares[i]

    own_rows = pl.ds(pl.multiple_of(me * rows, rows), rows)
    for i, (update, weight, copy) in enumerate(
        ((update_q, weight_q, copy_q), (update_v, weight_v, copy_v))
    ):
        scale = jnp.sqrt(
            tile[2 * i : 2 * i + 1, :1] / (tile[2 * i + 1 : 2 * i + 2, :1] + epsilon)
        )
        scaled = scale * update[...]
        update[...] = scaled
        copy[own_rows, :] = (weight[...] - learning_rate * scaled).astype(bf16)

    def rows_of(device):
        return pl.ds(pl.multiple_of(device * rows, rows), rows)

    def z_copies(k):
        where = rows_of(me)
        peer = (((z + k) % nz) * ny + y, tp)
        return [
            remote(c.at[where, :], c.at[where, :], z_sems.at[0, i, k - 1], z_sems.at[1, i, k - 1], peer)
            for i, c in enumerate((copy_q, copy_v))
        ]

    def y_copies(d, k):
        where = rows_of(((z + nz - k) % nz) * ny + y)
        peer = (z * ny + (y + d) % ny, tp)
        n = (d - 1) * nz + k
        return [
            remote(c.at[where, :], c.at[where, :], y_sems.at[0, i, n], y_sems.at[1, i, n], peer)
            for i, c in enumerate((copy_q, copy_v))
        ]

    order = sorted(range(1, nz), key=lambda k: min(k, nz - k))
    for k in order:
        for copy in z_copies(k):
            copy.start()
    for d in range(1, ny):
        for copy in y_copies(d, 0):
            copy.start()

    for copy in left_copies + right_copies:
        copy.wait_recv()

    def add_up(terms, count, picked):
        total = terms[0, picked].astype(f32)
        for i in range(1, count):
            total = total + terms[i, picked].astype(f32)
        return total

    for new, stat, first, columns in (
        (left_new_q, left_stat_q, 0, width_q * ntp),
        (left_new_v, left_stat_v, blocks, width_v * ntp),
    ):
        for b in range(blocks):
            total = add_up(left_terms, ntp, first + b)
            new[b] = statistic_decay * stat[b] + (1.0 - statistic_decay) / columns * total
    for new, stat, first in ((right_new_q, right_stat_q, 0), (right_new_v, right_stat_v, heads_q)):
        for h in range(stat.shape[0]):
            total = add_up(right_terms, nfs, first + h)
            new[h] = statistic_decay * stat[h] + (1.0 - statistic_decay) / (rows * nfs) * total

    for k in order:
        for copy in z_copies(k):
            copy.wait_recv()
        for d in range(1, ny):
            for copy in y_copies(d, k):
                copy.start()
    for d in range(1, ny):
        for k in range(nz):
            for copy in y_copies(d, k):
                copy.wait()
    for k in order:
        for copy in z_copies(k):
            copy.wait_send()
    for copy in tp_copies + fs_copies + left_copies + right_copies:
        copy.wait_send()


def block_diagonal(root):
    count, head = root.shape[:2]
    same = jnp.arange(count)[:, None, None, None] == jnp.arange(count)[None, None, :, None]
    return jnp.where(same, root[:, :, None, :], 0).reshape(count * head, count * head)


def local(
    nfs,
    ntp,
    layer_input,
    query_cotangent,
    value_cotangent,
    query_weight,
    value_weight,
    query_moment,
    value_moment,
    query_left_stat,
    value_left_stat,
    query_right_stat,
    value_right_stat,
    query_left_root,
    value_left_root,
    query_right_root,
    value_right_root,
):
    nz, ny = grid_of(nfs)
    cotangent = jnp.concatenate([query_cotangent.T, value_cotangent.T], axis=0)
    gradient = gradients_of_rows(nz, ny, cotangent, layer_input)
    rows, width_q = query_weight.shape
    width_v = value_weight.shape[1]
    left_shape, right_q, right_v = query_left_stat.shape, query_right_stat.shape, value_right_stat.shape
    head_count = right_q[0] + right_v[0]
    shape = jax.ShapeDtypeStruct
    dma = pltpu.SemaphoreType.DMA
    vmem = pl.BlockSpec(memory_space=pltpu.VMEM)
    return pl.pallas_call(
        functools.partial(update_kernel, nz, ny, ntp),
        out_shape=(
            shape((rows, width_q), f32),
            shape((rows, width_v), f32),
            shape((rows, width_q), f32),
            shape((rows, width_v), f32),
            shape(left_shape, f32),
            shape(left_shape, f32),
            shape(right_q, f32),
            shape(right_v, f32),
            shape((rows * nfs, width_q), bf16),
            shape((rows * nfs, width_v), bf16),
        ),
        in_specs=[vmem] * 13,
        out_specs=(vmem,) * 10,
        scratch_shapes=[
            pltpu.VMEM((ntp, 2 * left_shape[0]) + left_shape[1:], bf16),
            pltpu.VMEM((nfs, head_count) + right_q[1:], bf16),
            pltpu.VMEM((ntp, 8, 128), f32),
            pltpu.VMEM((nfs, 8, 128), f32),
            dma((2, ntp - 1)),
            dma((2, nfs - 1)),
            dma((2, ntp - 1)),
            dma((2, nfs - 1)),
            dma((2, 2, nz - 1)),
            dma((2, 2, (ny - 1) * nz)),
        ],
        compiler_params=pltpu.CompilerParams(collective_id=1, has_side_effects=True),
    )(
        gradient,
        query_weight,
        value_weight,
        query_moment,
        value_moment,
        query_left_stat,
        value_left_stat,
        query_right_stat,
        value_right_stat,
        query_left_root,
        value_left_root,
        block_diagonal(query_right_root),
        block_diagonal(value_right_root),
    )


def solution(mesh):
    matrix, left, right = P("fs", "tp"), P("fs", None, None), P("tp", None, None)
    return jax.shard_map(
        functools.partial(local, mesh.shape["fs"], mesh.shape["tp"]),
        mesh=mesh,
        in_specs=(P("fs", None),) + (matrix,) * 6 + (left, left, right, right) * 2,
        out_specs=(matrix,) * 4 + (left, left, right, right) + (P(None, "tp"),) * 2,
        check_vma=False,
    )
```

```python
import functools

import jax
import jax.numpy as jnp
from jax import lax
from jax.experimental import pallas as pl
from jax.experimental.pallas import tpu as pltpu
from jax.sharding import PartitionSpec as P

MESH = pl.DeviceIdType.MESH
f32 = jnp.float32
bf16 = jnp.bfloat16

momentum_decay = 0.9
statistic_decay = 0.9
learning_rate = 0.002
epsilon = 1e-06


def grid_of(fs):
    nz = 4 if fs % 4 == 0 else 1
    return nz, fs // nz


def greet(peers):
    barrier = pltpu.get_barrier_semaphore()
    for peer in peers:
        pl.semaphore_signal(barrier, inc=1, device_id=peer, device_id_type=MESH)
    pl.semaphore_wait(barrier, len(peers))


def remote(src, dst, send_sem, recv_sem, peer):
    return pltpu.make_async_remote_copy(
        src_ref=src,
        dst_ref=dst,
        send_sem=send_sem,
        recv_sem=recv_sem,
        device_id=peer,
        device_id_type=MESH,
    )


def mix(moment, gradient):
    return momentum_decay * moment + (1.0 - momentum_decay) * gradient


def gradient_kernel(
    nz,
    ny,
    cot_ref,
    x_ref,
    out_ref,
    xbuf,
    far,
    far_in,
    near,
    hop,
    hop_in,
    x_sem,
    y_send,
    y_recv,
    z_send,
    z_recv,
):
    me, tp = lax.axis_index("fs"), lax.axis_index("tp")
    z, y = me // ny, me % ny
    rows = out_ref.shape[1]
    chunks, far_count = nz * ny, nz * (ny - 1)
    slots = xbuf.shape[0]

    def owner(i):
        return ((z + i % nz + 1) % nz) * ny + (y + i // nz + 1) % ny

    def fetch(i):
        columns = pl.ds(pl.multiple_of(owner(i) * rows, 128), rows)
        return pltpu.make_async_copy(
            x_ref.at[:, columns], xbuf.at[i % slots], x_sem.at[i % slots]
        )

    def y_copy(i):
        peer = (z * ny + (y + i // nz + 1) % ny, tp)
        return remote(far.at[i], far_in.at[i], y_send.at[i], y_recv.at[i], peer)

    def z_copy(k):
        peer = (((z + k + 1) % nz) * ny + y, tp)
        return remote(hop.at[k], hop_in.at[k], z_send.at[k], z_recv.at[k], peer)

    for i in range(slots - 1):
        fetch(i).start()
    peers = [(z * ny + (y + d) % ny, tp) for d in range(1, ny)]
    peers += [(((z + d) % nz) * ny + y, tp) for d in range(1, nz)]
    greet(peers)

    width = min(rows, 256)

    def multiply(i, keep):
        @pl.when(i + slots - 1 < chunks)
        def _():
            fetch(i + slots - 1).start()

        fetch(i).wait()
        for j in range(rows // width):
            part = jnp.dot(
                cot_ref[...],
                xbuf[i % slots, :, j * width : (j + 1) * width],
                preferred_element_type=f32,
            )
            keep(i, slice(j * width, (j + 1) * width), part)

    def far_step(i, carry):
        def keep(i, columns, part):
            far[i, :, columns] = part.astype(bf16)

        multiply(i, keep)
        y_copy(i).start()
        return carry

    def near_step(i, carry):
        def keep(i, columns, part):
            near[i - far_count, :, columns] = part

        multiply(i, keep)
        return carry

    lax.fori_loop(0, far_count, far_step, 0)
    lax.fori_loop(far_count, chunks, near_step, 0)

    for k in range(nz):
        for d in range(ny - 1):
            y_copy(d * nz + k).wait_recv()
        total = near[k]
        for d in range(ny - 1):
            total = total + far_in[d * nz + k].astype(f32)
        if k < nz - 1:
            hop[k] = total.astype(bf16)
            z_copy(k).start()
        else:
            out_ref[...] = total
    for k in range(nz - 1):
        z_copy(k).wait_recv()
        out_ref[...] += hop_in[k].astype(f32)
    for i in range(far_count):
        y_copy(i).wait_send()
    for k in range(nz - 1):
        z_copy(k).wait_send()


def gradients_of_rows(nz, ny, cotangent, layer_input):
    columns, tokens = cotangent.shape
    rows = layer_input.shape[1] // (nz * ny)
    far_count = nz * (ny - 1)
    return pl.pallas_call(
        functools.partial(gradient_kernel, nz, ny),
        out_shape=jax.ShapeDtypeStruct((columns, rows), f32),
        in_specs=[
            pl.BlockSpec(memory_space=pltpu.VMEM),
            pl.BlockSpec(memory_space=pl.ANY),
        ],
        out_specs=pl.BlockSpec(memory_space=pltpu.VMEM),
        scratch_shapes=[
            pltpu.VMEM((3, tokens, rows), bf16),
            pltpu.VMEM((far_count, columns, rows), bf16),
            pltpu.VMEM((far_count, columns, rows), bf16),
            pltpu.VMEM((nz, columns, rows), f32),
            pltpu.VMEM((nz - 1, columns, rows), bf16),
            pltpu.VMEM((nz - 1, columns, rows), bf16),
            pltpu.SemaphoreType.DMA((3,)),
            pltpu.SemaphoreType.DMA((far_count,)),
            pltpu.SemaphoreType.DMA((far_count,)),
            pltpu.SemaphoreType.DMA((nz - 1,)),
            pltpu.SemaphoreType.DMA((nz - 1,)),
        ],
        compiler_params=pltpu.CompilerParams(collective_id=0, has_side_effects=True),
    )(cotangent, layer_input)


def dot_split(left, right, split_left):
    wide = left if split_left else right
    high = wide.astype(bf16)
    low = (wide - high.astype(f32)).astype(bf16)
    if split_left:
        return jnp.dot(high, right, preferred_element_type=f32) + jnp.dot(
            low, right, preferred_element_type=f32
        )
    return jnp.dot(left, high, preferred_element_type=f32) + jnp.dot(
        left, low, preferred_element_type=f32
    )


def outer(a):
    return lax.dot_general(a, a, (((1,), (1,)), ((), ())), preferred_element_type=f32)


def total_of(x):
    return jnp.sum(jnp.sum(x, axis=0, keepdims=True), axis=1, keepdims=True)


def update_kernel(
    nz,
    ny,
    ntp,
    grad_ref,
    weight_q,
    weight_v,
    moment_q,
    moment_v,
    left_stat_q,
    left_stat_v,
    right_stat_q,
    right_stat_v,
    left_root_q,
    left_root_v,
    right_root_q,
    right_root_v,
    update_q,
    update_v,
    moment_new_q,
    moment_new_v,
    left_new_q,
    left_new_v,
    right_new_q,
    right_new_v,
    copy_q,
    copy_v,
    left_terms,
    right_terms,
    tp_squares,
    fs_squares,
    tp_sems,
    fs_sems,
    left_sems,
    right_sems,
    z_sems,
    y_sems,
):
    nfs = nz * ny
    me, tp = lax.axis_index("fs"), lax.axis_index("tp")
    z, y = me // ny, me % ny
    rows, width_q = moment_q.shape
    width_v = moment_v.shape[1]
    blocks, block = left_root_q.shape[:2]
    head = right_stat_q.shape[1]
    heads_q, heads_v = right_stat_q.shape[0], right_stat_v.shape[0]

    tp_peers = [(me, (tp + d) % ntp) for d in range(1, ntp)]
    fs_peers = [((me + d) % nfs, tp) for d in range(1, nfs)]

    def direction(grad, moment, moment_new, left_root, right_root, update):
        new = mix(moment[...], grad)
        moment_new[...] = new
        turned = dot_split(new, right_root[...], True)
        squares = jnp.zeros((1, 1), f32)
        for b in range(blocks):
            part = dot_split(left_root[b], turned[b * block : (b + 1) * block], False)
            update[b * block : (b + 1) * block, :] = part
            squares = squares + total_of(part * part)
        return total_of(new * new), squares

    grad_q = grad_ref[:width_q, :].T
    grad_v = grad_ref[width_q:, :].T
    sums = direction(grad_q, moment_q, moment_new_q, left_root_q, right_root_q, update_q)
    sums += direction(grad_v, moment_v, moment_new_v, left_root_v, right_root_v, update_v)
    row = lax.broadcasted_iota(jnp.int32, (8, 128), 0)
    tile = jnp.zeros((8, 128), f32)
    for i, one in enumerate(sums):
        tile = jnp.where(row == i, one, tile)
    tp_squares[tp] = tile

    greet(tp_peers + fs_peers)

    def spread(buffer, own, sems, peers):
        return [
            remote(buffer.at[own], buffer.at[own], sems.at[0, d], sems.at[1, d], peer)
            for d, peer in enumerate(peers)
        ]

    tp_copies = spread(tp_squares, tp, tp_sems, tp_peers)
    fs_copies = spread(fs_squares, me, fs_sems, fs_peers)
    left_copies = spread(left_terms, tp, left_sems, tp_peers)
    right_copies = spread(right_terms, me, right_sems, fs_peers)

    for copy in tp_copies:
        copy.start()
    for grad, first in ((grad_q, 0), (grad_v, blocks)):
        narrow = grad.astype(bf16)
        for b in range(blocks):
            left_terms[tp, first + b] = outer(narrow[b * block : (b + 1) * block]).astype(bf16)
    for h in range(heads_q + heads_v):
        right_terms[me, h] = outer(grad_ref[h * head : (h + 1) * head, :].astype(bf16)).astype(bf16)
    for copy in tp_copies:
        copy.wait_recv()
    tile = tp_squares[0]
    for i in range(1, ntp):
        tile = tile + tp_squares[i]
    fs_squares[me] = tile
    for copy in fs_copies + left_copies:
        copy.start()
    for copy in fs_copies:
        copy.wait_recv()
    tile = fs_squares[0]
    for i in range(1, nfs):
        tile = tile + fs_squares[i]

    own_rows = pl.ds(pl.multiple_of(me * rows, rows), rows)
    for i, (update, weight, copy) in enumerate(
        ((update_q, weight_q, copy_q), (update_v, weight_v, copy_v))
    ):
        scale = jnp.sqrt(
            tile[2 * i : 2 * i + 1, :1] / (tile[2 * i + 1 : 2 * i + 2, :1] + epsilon)
        )
        scaled = scale * update[...]
        update[...] = scaled
        copy[own_rows, :] = (weight[...] - learning_rate * scaled).astype(bf16)

    def rows_of(device):
        return pl.ds(pl.multiple_of(device * rows, rows), rows)

    def z_copies(k):
        where = rows_of(me)
        peer = (((z + k) % nz) * ny + y, tp)
        return [
            remote(c.at[where, :], c.at[where, :], z_sems.at[0, i, k - 1], z_sems.at[1, i, k - 1], peer)
            for i, c in enumerate((copy_q, copy_v))
        ]

    def y_copies(d, k):
        where = rows_of(((z + nz - k) % nz) * ny + y)
        peer = (z * ny + (y + d) % ny, tp)
        n = (d - 1) * nz + k
        return [
            remote(c.at[where, :], c.at[where, :], y_sems.at[0, i, n], y_sems.at[1, i, n], peer)
            for i, c in enumerate((copy_q, copy_v))
        ]

    order = sorted(range(1, nz), key=lambda k: min(k, nz - k))
    for k in order:
        for copy in z_copies(k):
            copy.start()
    for d in range(1, ny):
        for copy in y_copies(d, 0):
            copy.start()

    for copy in right_copies:
        copy.start()
    for k in order:
        for copy in z_copies(k):
            copy.wait_recv()
        for d in range(1, ny):
            for copy in y_copies(d, k):
                copy.start()
    for copy in left_copies + right_copies:
        copy.wait_recv()

    def add_up(terms, count, picked):
        total = terms[0, picked].astype(f32)
        for i in range(1, count):
            total = total + terms[i, picked].astype(f32)
        return total

    for new, stat, first, columns in (
        (left_new_q, left_stat_q, 0, width_q * ntp),
        (left_new_v, left_stat_v, blocks, width_v * ntp),
    ):
        for b in range(blocks):
            total = add_up(left_terms, ntp, first + b)
            new[b] = statistic_decay * stat[b] + (1.0 - statistic_decay) / columns * total
    for new, stat, first in ((right_new_q, right_stat_q, 0), (right_new_v, right_stat_v, heads_q)):
        for h in range(stat.shape[0]):
            total = add_up(right_terms, nfs, first + h)
            new[h] = statistic_decay * stat[h] + (1.0 - statistic_decay) / (rows * nfs) * total

    for d in range(1, ny):
        for k in range(nz):
            for copy in y_copies(d, k):
                copy.wait()
    for k in order:
        for copy in z_copies(k):
            copy.wait_send()
    for copy in tp_copies + fs_copies + left_copies + right_copies:
        copy.wait_send()


def block_diagonal(root):
    count, head = root.shape[:2]
    same = jnp.arange(count)[:, None, None, None] == jnp.arange(count)[None, None, :, None]
    return jnp.where(same, root[:, :, None, :], 0).reshape(count * head, count * head)


def local(
    nfs,
    ntp,
    layer_input,
    query_cotangent,
    value_cotangent,
    query_weight,
    value_weight,
    query_moment,
    value_moment,
    query_left_stat,
    value_left_stat,
    query_right_stat,
    value_right_stat,
    query_left_root,
    value_left_root,
    query_right_root,
    value_right_root,
):
    nz, ny = grid_of(nfs)
    cotangent = jnp.concatenate([query_cotangent.T, value_cotangent.T], axis=0)
    gradient = gradients_of_rows(nz, ny, cotangent, layer_input)
    rows, width_q = query_weight.shape
    width_v = value_weight.shape[1]
    left_shape, right_q, right_v = query_left_stat.shape, query_right_stat.shape, value_right_stat.shape
    head_count = right_q[0] + right_v[0]
    shape = jax.ShapeDtypeStruct
    dma = pltpu.SemaphoreType.DMA
    vmem = pl.BlockSpec(memory_space=pltpu.VMEM)
    return pl.pallas_call(
        functools.partial(update_kernel, nz, ny, ntp),
        out_shape=(
            shape((rows, width_q), f32),
            shape((rows, width_v), f32),
            shape((rows, width_q), f32),
            shape((rows, width_v), f32),
            shape(left_shape, f32),
            shape(left_shape, f32),
            shape(right_q, f32),
            shape(right_v, f32),
            shape((rows * nfs, width_q), bf16),
            shape((rows * nfs, width_v), bf16),
        ),
        in_specs=[vmem] * 13,
        out_specs=(vmem,) * 10,
        scratch_shapes=[
            pltpu.VMEM((ntp, 2 * left_shape[0]) + left_shape[1:], bf16),
            pltpu.VMEM((nfs, head_count) + right_q[1:], bf16),
            pltpu.VMEM((ntp, 8, 128), f32),
            pltpu.VMEM((nfs, 8, 128), f32),
            dma((2, ntp - 1)),
            dma((2, nfs - 1)),
            dma((2, ntp - 1)),
            dma((2, nfs - 1)),
            dma((2, 2, nz - 1)),
            dma((2, 2, (ny - 1) * nz)),
        ],
        compiler_params=pltpu.CompilerParams(collective_id=1, has_side_effects=True),
    )(
        gradient,
        query_weight,
        value_weight,
        query_moment,
        value_moment,
        query_left_stat,
        value_left_stat,
        query_right_stat,
        value_right_stat,
        query_left_root,
        value_left_root,
        block_diagonal(query_right_root),
        block_diagonal(value_right_root),
    )


def solution(mesh):
    matrix, left, right = P("fs", "tp"), P("fs", None, None), P("tp", None, None)
    return jax.shard_map(
        functools.partial(local, mesh.shape["fs"], mesh.shape["tp"]),
        mesh=mesh,
        in_specs=(P("fs", None),) + (matrix,) * 6 + (left, left, right, right) * 2,
        out_specs=(matrix,) * 4 + (left, left, right, right) + (P(None, "tp"),) * 2,
        check_vma=False,
    )
```
